32 devices in a mesh: gr: 2 (over x), fs: 8 (over z, y), tp: 2 (over core).
Axes of the slice: x: 2, y: 2, z: 4, core: 2. Of those that a mesh axis runs over, the one named last changes fastest.
Arguments:
- tokens: bfloat16 [16384, 3072], P(('gr', 'fs')), may hold values from -6 to 6
- norm_gain: float32 [3072], P(('gr', 'fs')), may hold values from 0.1 to 1.9
- gate_weight: float32 [8, 3072, 768], P(None, ('gr', 'fs'), 'tp'), may hold values from -0.109375 to 0.109375
- up_weight: float32 [8, 3072, 768], P(None, ('gr', 'fs'), 'tp'), may hold values from -0.109375 to 0.109375
- down_weight: float32 [8, 3072, 768], P(None, ('gr', 'fs'), 'tp'), may hold values from -0.21875 to 0.21875
- group_pick: int32 [16384], P(('gr', 'fs')), may hold values from 0 to 3, as said below
- expert_pick: int32 [16384, 2], P(('gr', 'fs')), may hold values from 0 to 1, as said below
- route_weight: float32 [16384, 2], P(('gr', 'fs')), may hold values from 0.1 to 1
Outputs:
- combined: bfloat16 [16384, 3072], P(('gr', 'fs'), 'tp')
- gate_served: bfloat16 [8, 3072, 768], P('fs', None, 'tp')
- up_served: bfloat16 [8, 3072, 768], P('fs', None, 'tp')
- down_served: bfloat16 [8, 3072, 768], P('fs', None, 'tp')
The draws below stay inside these ranges and needn't reach their ends.
Inputs may be any that keep to these rules, and one draw needn't show every extreme that they name: `group_pick`: in each aligned block of 1024 rows every group is picked by the same number of rows. `expert_pick`: the 2 entries of a row differ. In each aligned block of 1024 rows, every expert (group and number together) is named exactly 256 times.
All inputs are finite; a program needn't handle non-finite values.
Results may differ from the reference program's by a relative error of at most 0.0092.
Values may be sent and summed in bfloat16 or wider, within the bound.
A program may use at most 128 MiB of HBM per device.

```python
import math
import jax
import jax.numpy as jnp
from jax import lax

D = 3072
FF = 768
GROUPS = 4
TOP = 2
TOK_DEV = 1024
EXPERTS = 8
TOKENS = 16384
N_TP = 2


def routing(key):
    blocks = TOKENS // TOK_DEV
    per_group = EXPERTS // GROUPS
    position = jnp.arange(TOK_DEV, dtype=jnp.int32)
    group_of = position % GROUPS
    within = position // GROUPS
    first_pick = within % per_group
    second_pick = (first_pick + 1 + within // per_group % (per_group - 1)) % per_group

    def one_block(block_key):
        order_key, label_key = jax.random.split(block_key)
        order = jax.random.permutation(order_key, TOK_DEV)
        relabel = jax.vmap(lambda label_one: jax.random.permutation(label_one, per_group))(jax.random.split(label_key, GROUPS))
        first_label = relabel[group_of, first_pick]
        second_label = relabel[group_of, second_pick]
        pairs = jnp.stack([first_label, second_label], axis=1).astype(jnp.int32)
        group_tok = jnp.zeros((TOK_DEV,), jnp.int32).at[order].set(group_of)
        pair_tok = jnp.zeros((TOK_DEV, 2), jnp.int32).at[order].set(pairs)
        return (group_tok, pair_tok)
    block_keys = jax.random.split(jax.random.fold_in(key, 71), blocks)
    groups_all, pairs_all = jax.vmap(one_block)(block_keys)
    return (groups_all.reshape(TOKENS).astype(jnp.int32), pairs_all.reshape(TOKENS, 2).astype(jnp.int32))


def draw_group_pick(key, part):
    return routing(key)[0]


def draw_expert_pick(key, part):
    return routing(key)[1]


def block_levels(own_key, dims, pieces, low, high):
    def one(dim, shards_of):
        heights = jax.random.uniform(jax.random.fold_in(jax.random.fold_in(own_key, 6), dim), (shards_of,), jnp.float32, low / len(pieces), high / len(pieces))
        return jnp.repeat(jnp.exp(heights), dims[dim] // shards_of).reshape((-1,) + (1,) * (len(dims) - dim - 1))

    loudness = one(*pieces[0])
    for cut in pieces[1:]:
        loudness = loudness * one(*cut)
    return loudness


def centred(own_key, extent, spread, bound, pieces=(), held_as=jnp.bfloat16):
    result = jax.random.normal(own_key, extent, jnp.float32) * spread
    if len(pieces) > 0:
        result = block_levels(own_key, extent, pieces, -0.22, 0.18) * result
    return jnp.clip(result, min=-bound, max=bound).astype(held_as)


def setup_inputs(seed: int = 0) -> dict:
    key_of = jax.random.split(jax.random.key(seed), 9)
    return {
        "tokens": centred(key_of[0], (TOKENS, D), 1.0, 6.0, ((0, 16),)),
        "norm_gain": jnp.clip(1.0 + 0.18 * jax.random.normal(key_of[1], (D,), jnp.float32), 0.1, 1.9),
        "gate_weight": centred(key_of[2], (EXPERTS, D, FF), D ** -0.5, 0.109375, ((1, 16), (2, 2)), jnp.float32),
        "up_weight": centred(key_of[3], (EXPERTS, D, FF), D ** -0.5, 0.109375, ((1, 16), (2, 2)), jnp.float32),
        "down_weight": centred(key_of[4], (EXPERTS, D, FF), FF ** -0.5, 0.21875, ((1, 16), (2, 2)), jnp.float32),
        "group_pick": draw_group_pick(jax.random.fold_in(key_of[8], 71), 0),
        "expert_pick": draw_expert_pick(jax.random.fold_in(key_of[8], 71), 0),
        "route_weight": jnp.clip(jnp.exp(math.log(1.0) - 2.3025851 * jax.random.uniform(key_of[7], (TOKENS, TOP), jnp.float32) ** block_levels(key_of[7], (TOKENS, TOP), ((0, 16),), -0.2, 0.2)), 0.1, 1.0),
    }


EPS = 1e-06

def reference(tokens, norm_gain, gate_weight, up_weight, down_weight, group_pick, expert_pick, route_weight):
    gate_served = (norm_gain[None, :, None] * gate_weight).astype(jnp.bfloat16)
    up_served = (norm_gain[None, :, None] * up_weight).astype(jnp.bfloat16)
    down_served = down_weight.astype(jnp.bfloat16)
    as_float = tokens.astype(jnp.float32)
    normed = (as_float * lax.rsqrt(lax.optimization_barrier(jnp.mean(as_float * as_float, axis=-1, keepdims=True)) + EPS)).astype(jnp.bfloat16)
    expert_ids = (group_pick[:, None] * (EXPERTS // GROUPS) + expert_pick).reshape(-1).astype(jnp.int32)
    per_expert = TOP * TOKENS // EXPERTS
    half_width = FF // N_TP

    def run_expert(expert_item):
        w_gate, w_up, w_down, index = expert_item
        row_ids = jnp.nonzero(expert_ids == index, size=per_expert)[0]
        rows_in = normed[row_ids // TOP]
        gate_acts = jnp.dot(rows_in, w_gate, preferred_element_type=jnp.float32)
        up_acts = jnp.dot(rows_in, w_up, preferred_element_type=jnp.float32)
        hidden = (jax.nn.silu(gate_acts) * up_acts).astype(jnp.bfloat16)
        accum_sum = jnp.zeros((per_expert, D), jnp.float32)
        for block in range(N_TP):
            part_sum = lax.dot_general(hidden[:, block * half_width:(block + 1) * half_width], w_down[:, block * half_width:(block + 1) * half_width], (((1,), (1,)), ((), ())), preferred_element_type=jnp.float32)
            accum_sum = accum_sum + lax.optimization_barrier(part_sum.astype(jnp.bfloat16)).astype(jnp.float32)
        return (accum_sum.astype(jnp.bfloat16), row_ids)
    outputs, row_ids = lax.map(run_expert, (gate_served, up_served, down_served, jnp.arange(EXPERTS, dtype=jnp.int32)))
    flat_out = jnp.zeros((TOP * TOKENS, D), jnp.bfloat16).at[row_ids.reshape(-1)].set(outputs.reshape(-1, D))
    combined = lax.optimization_barrier(jnp.sum(route_weight[:, :, None] * flat_out.reshape(TOKENS, TOP, D).astype(jnp.float32), axis=1))
    return (combined.astype(jnp.bfloat16), gate_served, up_served, down_served)
```

```python
import jax
import jax.numpy as jnp
from jax import lax
from jax.experimental import pallas as pl
from jax.experimental.pallas import tpu as pltpu
from jax.sharding import PartitionSpec as P

GROUPS = 4


EPS = 1e-06


def local_spread(
    tokens, norm_gain, gate_weight, up_weight, down_weight, group_pick, expert_pick, route_weight
):
    scaled = norm_gain[None, :, None]
    gate_local = (scaled * gate_weight).astype(jnp.bfloat16)
    up_local = (scaled * up_weight).astype(jnp.bfloat16)
    down_local = down_weight.astype(jnp.bfloat16)
    experts, rows_dev, cols_dev = gate_local.shape
    gate_four = gate_local.reshape(experts, 1, rows_dev, cols_dev)
    up_four = up_local.reshape(experts, 1, rows_dev, cols_dev)
    down_four = down_local.reshape(experts, 1, rows_dev, cols_dev)
    gathered = (
        lax.all_gather(gate_four, "gr", axis=1, tiled=True),
        lax.all_gather(up_four, "gr", axis=1, tiled=True),
        lax.all_gather(down_four, "gr", axis=1, tiled=True),
    )
    relaid = (
        lax.all_to_all(gathered[0], "fs", split_axis=0, concat_axis=2, tiled=True),
        lax.all_to_all(gathered[1], "fs", split_axis=0, concat_axis=2, tiled=True),
        lax.all_to_all(gathered[2], "fs", split_axis=0, concat_axis=2, tiled=True),
    )
    gate_new = relaid[0].reshape(1, -1, cols_dev)
    up_new = relaid[1].reshape(1, -1, cols_dev)
    down_new = relaid[2].reshape(1, -1, cols_dev)
    tok_rows, model_width = tokens.shape
    as_float = tokens.astype(jnp.float32)
    normed = (
        as_float * lax.rsqrt(jnp.mean(as_float * as_float, axis=-1, keepdims=True) + EPS)
    ).astype(jnp.bfloat16)
    per_group = experts // GROUPS
    top_count = expert_pick.shape[1]
    capacity = top_count * tok_rows // experts
    flat_ids = (group_pick[:, None] * per_group + expert_pick).reshape(-1)
    onehot = (flat_ids[:, None] == jnp.arange(experts, dtype=jnp.int32)[None, :]).astype(jnp.int32)
    slot_index = jnp.sum(onehot * (jnp.cumsum(onehot, axis=0) - 1), axis=1)
    target = flat_ids * capacity + slot_index
    source = (
        jnp.zeros((experts * capacity,), jnp.int32)
        .at[target]
        .set(jnp.arange(top_count * tok_rows, dtype=jnp.int32) // top_count)
    )
    outgoing = normed[source].reshape(experts, capacity, model_width)
    share = capacity // lax.axis_size("tp")
    start = lax.axis_index("tp") * share
    my_share = lax.dynamic_slice_in_dim(outgoing, start, share, 1)
    landed = lax.all_to_all(my_share, "fs", split_axis=0, concat_axis=1, tiled=True).reshape(
        experts, share, model_width
    )
    arrived = lax.all_gather(landed, "tp", axis=1, tiled=True).reshape(-1, model_width)
    gate_acts = jnp.dot(arrived, gate_new[0], preferred_element_type=jnp.float32)
    up_acts = jnp.dot(arrived, up_new[0], preferred_element_type=jnp.float32)
    hidden = (jax.nn.silu(gate_acts) * up_acts).astype(jnp.bfloat16)
    partial_value = lax.dot_general(
        hidden, down_new[0], (((1,), (1,)), ((), ())), preferred_element_type=jnp.float32
    ).astype(jnp.bfloat16)
    summed = (
        lax.psum_scatter(partial_value, "tp", scatter_dimension=1, tiled=True)
        .astype(jnp.float32)
        .astype(jnp.bfloat16)
    )
    returned = lax.all_to_all(summed, "fs", split_axis=0, concat_axis=0, tiled=True)
    picked = returned[target].reshape(tok_rows, top_count, -1).astype(jnp.float32)
    combined = jnp.sum(route_weight[:, :, None] * picked, axis=1).astype(jnp.bfloat16)
    return (combined, gate_new, up_new, down_new)


def greet(peers):
    barrier = pltpu.get_barrier_semaphore()
    for peer in peers:
        pl.semaphore_signal(barrier, inc=1, device_id=peer, device_id_type=pl.DeviceIdType.MESH)
    pl.semaphore_wait(barrier, len(peers))


def remote(src, dst, send, recv, peer):
    return pltpu.make_async_remote_copy(
        src_ref=src,
        dst_ref=dst,
        send_sem=send,
        recv_sem=recv,
        device_id=peer,
        device_id_type=pl.DeviceIdType.MESH,
    )


def nearest_first(n):
    return [sorted(range(n), key=lambda z, g=g: (abs(z - g), z)) for g in range(n)]


def dot_nt(a, b):
    return lax.dot_general(a, b, (((1,), (1,)), ((), ())), preferred_element_type=jnp.float32)


def fused(tokens, gain, gate, up, down, group_pick, expert_pick, route_weight):
    experts, rows, cols = gate.shape
    tok_rows, width = tokens.shape
    n_fs = lax.axis_size("fs")
    n_gr = lax.axis_size("gr")
    n = GROUPS
    members = experts // n
    cap = tok_rows // n
    half = cap // 2
    out_w = width // 2
    n_w = 3
    table = nearest_first(n)
    bf16, f32, i32 = jnp.bfloat16, jnp.float32, jnp.int32
    lanes = 128

    def kernel(
        tok_in, gain_ref, w_gate, w_up, w_down, gp_ref, ep_ref, rw_ref,
        out, s_gate, s_up, s_down,
        W, wf, ow, tok, outgoing, arrived, aw, pin, ownp, home, h, pcol, wout, wcol,
        sends, local, served, rwz, rwx, rwy, rdx, rdy, rtz, raz, rtt, rat, rp, rh,
    ):
        fs, gr, tp = lax.axis_index("fs"), lax.axis_index("gr"), lax.axis_index("tp")
        g, y = fs // members, fs % members
        other_y, other_x, other_t = 1 - y, 1 - gr, 1 - tp
        hit = [1 - ((g - c + n) % n + n - 1) // n for c in range(n)]
        zs = [sum(table[c][s] * hit[c] for c in range(n)) for s in range(n)]
        x_peer, y_peer, t_peer = {"gr": other_x}, {"fs": g * members + other_y}, {"tp": other_t}
        z_peers = [{"fs": zs[s] * members + y} for s in range(n)]
        started = []

        def send(src, dst, recv, peer):
            copy = remote(src, dst, sends.at[len(started)], recv, peer)
            copy.start()
            started.append(copy)

        def landed(ref, recv):
            remote(ref, ref, sends.at[0], recv, t_peer).wait_recv()

        def block(j, x, yy, z):
            at = pl.multiple_of((x * n_fs + z * members + yy) * rows, rows)
            return W.at[j, :, pl.ds(at, rows), :]

        w_in = (w_gate, w_up, w_down)
        loads = [
            [
                pltpu.make_async_copy(
                    w_in[w].at[pl.ds(zs[s] * members, members)], wf.at[w, s], local.at[s, w]
                )
                for w in range(n_w)
            ]
            for s in range(n)
        ]
        order = [1, 0] + list(range(2, n))
        for s in order:
            for copy in loads[s]:
                copy.start()
        tok_load = pltpu.make_async_copy(tok_in, tok, local.at[n, 0])
        tok_load.start()
        greet(z_peers[1:] + [x_peer, y_peer, t_peer])

        eye_r = lax.broadcasted_iota(i32, (rows, rows), 0)
        eye_c = lax.broadcasted_iota(i32, (rows, rows), 1)
        gain_col = jnp.sum(jnp.where(eye_r == eye_c, gain_ref[...], 0.0), axis=1, keepdims=True)

        def cast(s, j, w):
            value = wf[w, s, j]
            return ((gain_col * value) if w < 2 else value).astype(bf16)

        for s in order:
            for copy in loads[s]:
                copy.wait()
            for j in range(members):
                for w in range(n_w):
                    if s:
                        ow[s - 1, j, w] = cast(s, j, w)
                    else:
                        at = pl.multiple_of((gr * n_fs + fs) * rows, rows)
                        W[j, w, pl.ds(at, rows), :] = cast(s, j, w)
                if s:
                    send(ow.at[s - 1, j], block(j, gr, y, g), rwz.at[g, j], z_peers[s])
                else:
                    mine = block(j, gr, y, g)
                    send(mine, mine, rwx.at[g, j], x_peer)
                    send(mine, mine, rwy.at[g, j], y_peer)

        gp = gp_ref[...]
        onehot = jnp.where(
            lax.broadcasted_iota(i32, (16, tok_rows), 0) == gp, 1.0, 0.0
        )
        step = 256
        ranks = []
        for c in range(0, tok_rows, step):
            r_i = lax.broadcasted_iota(i32, (tok_rows, step), 0)
            c_i = lax.broadcasted_iota(i32, (tok_rows, step), 1) + c
            before = jnp.dot(
                onehot.astype(bf16),
                jnp.where(r_i < c_i, 1.0, 0.0).astype(bf16),
                preferred_element_type=f32,
            )
            ranks.append(jnp.sum(onehot[:, c : c + step] * before, axis=0, keepdims=True))
        place = gp.astype(f32) * cap + jnp.concatenate(ranks, axis=1)
        l_r = lax.broadcasted_iota(i32, (lanes, lanes), 0)
        l_c = lax.broadcasted_iota(i32, (lanes, lanes), 1)
        eye = l_r == l_c

        def column(row):
            return jnp.sum(jnp.where(eye, row, 0.0), axis=1, keepdims=True)

        for b in range(0, tok_rows, lanes):
            pcol[b : b + lanes, :] = column(place[:, b : b + lanes]).astype(i32)

        for m in range(members):
            value = jnp.zeros((1, tok_rows), f32)
            for k in range(members):
                value += jnp.where(ep_ref[k : k + 1, :] == m, rw_ref[k : k + 1, :], 0.0)
            for b in range(0, tok_rows, lanes):
                wcol[m, b : b + lanes, :] = column(value[:, b : b + lanes])
        place_i = place.astype(i32)

        tok_load.wait()

        def norm(i, _):
            at = pl.ds(pl.multiple_of(i * 64, 64), 64)
            x = tok[at, :].astype(f32)
            scale = lax.rsqrt(jnp.mean(x * x, axis=-1, keepdims=True) + EPS)
            tok[at, :] = (x * scale).astype(bf16)
            return 0

        lax.fori_loop(0, tok_rows // 64, norm, 0)

        first = pl.multiple_of(tp * half, half)
        for s in range(n):
            slots = lax.broadcasted_iota(i32, (half, tok_rows), 0) + (zs[s] * cap + tp * half)
            select = jnp.where(slots == place_i, 1.0, 0.0).astype(bf16)
            here = pcol[...] == lax.broadcasted_iota(i32, (tok_rows, half), 1) + (
                zs[s] * cap + tp * half
            )
            weights = jnp.zeros((8, half), f32)
            for m in range(members):
                row = jnp.sum(jnp.where(here, wcol[m], 0.0), axis=0, keepdims=True)
                weights = jnp.where(lax.broadcasted_iota(i32, (8, half), 0) == m, row, weights)
            span = 512
            target = arrived.at[g, pl.ds(first, half)] if s == 0 else outgoing.at[s - 1]

            def pick(c, _, target=target, select=select):
                at = pl.ds(pl.multiple_of(c * span, span), span)
                target[:, at] = jnp.dot(select, tok[:, at], preferred_element_type=f32).astype(bf16)
                return 0

            lax.fori_loop(0, width // span, pick, 0)
            if s == 0:
                aw[g, tp] = weights
                send(target, target, rtt.at[g], t_peer)
                send(aw.at[g, tp], aw.at[g, tp], rat.at[g], t_peer)
            else:
                wout[s - 1] = weights
                send(target, arrived.at[g, pl.ds(first, half)], rtz.at[g], z_peers[s])
                send(wout.at[s - 1], aw.at[g, tp], raz.at[g], z_peers[s])

        def relay(s):
            from_x, from_y = block(1, other_x, y, zs[s]), block(0, gr, other_y, zs[s])
            landed(from_x, rwx.at[zs[s], 1])
            send(from_x, from_x, rdy.at[zs[s]], y_peer)
            landed(from_y, rwy.at[zs[s], 0])
            send(from_y, from_y, rdx.at[zs[s]], x_peer)

        for s in range(1, n):
            for j in range(members):
                mine = block(j, gr, y, zs[s])
                landed(mine, rwz.at[zs[s], j])
                send(mine, mine, rwx.at[zs[s], j], x_peer)
                send(mine, mine, rwy.at[zs[s], j], y_peer)
            relay(s - 1)
        relay(n - 1)

        def forward(s):
            slot, small = arrived.at[zs[s], pl.ds(first, half)], aw.at[zs[s], tp]
            landed(slot, rtz.at[zs[s]])
            send(slot, slot, rtt.at[zs[s]], t_peer)
            landed(small, raz.at[zs[s]])
            send(small, small, rat.at[zs[s]], t_peer)

        forward(1)
        for s in range(n):
            landed(block(0, other_x, y, zs[s]), rwx.at[zs[s], 0])
            landed(block(1, gr, other_y, zs[s]), rwy.at[zs[s], 1])
            landed(block(0, other_x, other_y, zs[s]), rdx.at[zs[s]])
            landed(block(1, other_x, other_y, zs[s]), rdy.at[zs[s]])
        out_refs = (s_gate, s_up, s_down)
        stores = [
            pltpu.make_async_copy(W.at[y, w], out_refs[w], served.at[w]) for w in range(n_w)
        ]
        for copy in stores:
            copy.start()

        piece = 512
        second = pl.multiple_of(other_t * half, half)

        def chunk(s):
            z = zs[s]
            if s > 1:
                forward(s)
            landed(arrived.at[z, pl.ds(second, half)], rtt.at[z])
            landed(aw.at[z, other_t], rat.at[z])

            def act(j, _):
                rows_in = arrived[z]
                gate_acts = jnp.dot(rows_in, W[j, 0], preferred_element_type=f32)
                up_acts = jnp.dot(rows_in, W[j, 1], preferred_element_type=f32)
                value = gate_acts / (1.0 + jnp.exp(-gate_acts)) * up_acts
                for t in range(2):
                    scale = column(aw[z, t, pl.ds(j, 1), :])
                    at = slice(t * half, (t + 1) * half)
                    h[j, at, :] = (value[at] * scale).astype(bf16)
                return 0

            lax.fori_loop(0, members, act, 0)

            def down_rows(base, c):
                at = pl.ds(pl.multiple_of(base + c * piece, piece), piece)
                return dot_nt(h[0], W[0, 2, at, :]) + dot_nt(h[1], W[1, 2, at, :])

            give = tok.at[pl.ds(s * cap, cap), pl.ds(0, out_w)]
            back = tok.at[pl.ds(s * cap, cap), pl.ds(out_w, out_w)]

            def theirs(c, _):
                at = pl.ds(pl.multiple_of(c * piece, piece), piece)
                give[:, at] = down_rows(other_t * out_w, c).astype(bf16)
                return 0

            def ours(c, _):
                at = pl.ds(pl.multiple_of(c * piece, piece), piece)
                ownp[:, at] = down_rows(tp * out_w, c).astype(bf16).astype(f32)
                return 0

            lax.fori_loop(0, out_w // piece, theirs, 0)
            send(give, pin.at[s], rp.at[s], t_peer)
            lax.fori_loop(0, out_w // piece, ours, 0)
            landed(pin.at[s], rp.at[s])
            total = (ownp[...] + pin[s].astype(f32)).astype(bf16)
            if s:
                back[...] = total
                send(back, home.at[g], rh.at[g], z_peers[s])
            else:
                home[g] = total

        def restore(s):
            z = zs[s]

            def rows_of(b, _):
                at = pl.ds(pl.multiple_of(b * 256, 256), 256)
                slots = lax.broadcasted_iota(i32, (256, cap), 1) + z * cap
                back = jnp.where(slots == pcol[at, :], 1.0, 0.0).astype(bf16)
                value = jnp.dot(back, home[z], preferred_element_type=f32)
                if s:
                    value += out[at, :].astype(f32)
                out[at, :] = value.astype(bf16)
                return 0

            lax.fori_loop(0, tok_rows // 256, rows_of, 0)

        for s in [1, 2, 0] + list(range(3, n)):
            chunk(s)
        for s in range(n):
            if s:
                landed(home.at[zs[s]], rh.at[zs[s]])
            restore(s)
        for copy in stores:
            copy.wait()
        for copy in started:
            copy.wait_send()

    n_sends = (
        (n - 1) * members + 2 * members
        + 2 * n
        + (n - 1) * 2 * members + 2 * n
        + 2 * (n - 1)
        + n + n - 1
    )
    dma = pltpu.SemaphoreType.DMA
    vmem = pltpu.VMEM
    serve = jax.ShapeDtypeStruct((width, cols), bf16)
    any_space = pl.BlockSpec(memory_space=pl.ANY)
    in_vmem = pl.BlockSpec(memory_space=pltpu.VMEM)
    return pl.pallas_call(
        kernel,
        out_shape=(jax.ShapeDtypeStruct((tok_rows, out_w), bf16), serve, serve, serve),
        in_specs=[any_space, in_vmem, any_space, any_space, any_space] + [in_vmem] * 3,
        out_specs=(in_vmem, any_space, any_space, any_space),
        scratch_shapes=[
            vmem((members, n_w, width, cols), bf16),
            vmem((n_w, n, members, rows, cols), f32),
            vmem((n - 1, members, n_w, rows, cols), bf16),
            vmem((tok_rows, width), bf16),
            vmem((n - 1, half, width), bf16),
            vmem((n, cap, width), bf16),
            vmem((n, 2, 8, lanes), f32),
            vmem((n, cap, out_w), bf16),
            vmem((cap, out_w), f32),
            vmem((n, cap, out_w), bf16),
            vmem((members, cap, cols), bf16),
            vmem((tok_rows, 1), i32),
            vmem((n - 1, 8, lanes), f32),
            vmem((members, tok_rows, 1), f32),
            dma((n_sends,)),
            dma((n + 1, n_w)),
            dma((n_w,)),
            dma((n, members)),
            dma((n, members)),
            dma((n, members)),
            dma((n,)),
            dma((n,)),
            dma((n,)),
            dma((n,)),
            dma((n,)),
            dma((n,)),
            dma((n,)),
            dma((n,)),
        ],
        compiler_params=pltpu.CompilerParams(
            collective_id=0, has_side_effects=True, vmem_limit_bytes=63 * 2**20
        ),
        name="fused",
    )(
        tokens, gain[None, :], gate, up, down,
        group_pick[None, :], expert_pick.T, route_weight.T,
    )


def local_whole_group(*args):
    combined, gate_new, up_new, down_new = fused(*args)
    return (combined, gate_new[None], up_new[None], down_new[None])


def local(tokens, norm_gain, gate, up, down, group_pick, expert_pick, route_weight):
    per_group = gate.shape[0] // GROUPS
    fits = (
        per_group == expert_pick.shape[1] == 2
        and lax.axis_size("gr") == lax.axis_size("tp") == 2
        and lax.axis_size("fs") == gate.shape[0]
        and tokens.shape[0] == 2 * GROUPS * 128
    )
    body = local_whole_group if fits else local_spread
    return body(tokens, norm_gain, gate, up, down, group_pick, expert_pick, route_weight)


def solution(mesh):
    in_specs = (
        P(("gr", "fs"), None),
        P(("gr", "fs")),
        P(None, ("gr", "fs"), "tp"),
        P(None, ("gr", "fs"), "tp"),
        P(None, ("gr", "fs"), "tp"),
        P(("gr", "fs")),
        P(("gr", "fs"), None),
        P(("gr", "fs"), None),
    )
    out_specs = (
        P(("gr", "fs"), "tp"),
        P("fs", None, "tp"),
        P("fs", None, "tp"),
        P("fs", None, "tp"),
    )
    return jax.shard_map(local, mesh=mesh, in_specs=in_specs, out_specs=out_specs, check_vma=False)
```

```python
import jax
import jax.numpy as jnp
from jax import lax
from jax.experimental import pallas as pl
from jax.experimental.pallas import tpu as pltpu
from jax.sharding import PartitionSpec as P

GROUPS = 4


EPS = 1e-06


def local_spread(
    tokens, norm_gain, gate_weight, up_weight, down_weight, group_pick, expert_pick, route_weight
):
    scaled = norm_gain[None, :, None]
    gate_local = (scaled * gate_weight).astype(jnp.bfloat16)
    up_local = (scaled * up_weight).astype(jnp.bfloat16)
    down_local = down_weight.astype(jnp.bfloat16)
    experts, rows_dev, cols_dev = gate_local.shape
    gate_four = gate_local.reshape(experts, 1, rows_dev, cols_dev)
    up_four = up_local.reshape(experts, 1, rows_dev, cols_dev)
    down_four = down_local.reshape(experts, 1, rows_dev, cols_dev)
    gathered = (
        lax.all_gather(gate_four, "gr", axis=1, tiled=True),
        lax.all_gather(up_four, "gr", axis=1, tiled=True),
        lax.all_gather(down_four, "gr", axis=1, tiled=True),
    )
    relaid = (
        lax.all_to_all(gathered[0], "fs", split_axis=0, concat_axis=2, tiled=True),
        lax.all_to_all(gathered[1], "fs", split_axis=0, concat_axis=2, tiled=True),
        lax.all_to_all(gathered[2], "fs", split_axis=0, concat_axis=2, tiled=True),
    )
    gate_new = relaid[0].reshape(1, -1, cols_dev)
    up_new = relaid[1].reshape(1, -1, cols_dev)
    down_new = relaid[2].reshape(1, -1, cols_dev)
    tok_rows, model_width = tokens.shape
    as_float = tokens.astype(jnp.float32)
    normed = (
        as_float * lax.rsqrt(jnp.mean(as_float * as_float, axis=-1, keepdims=True) + EPS)
    ).astype(jnp.bfloat16)
    per_group = experts // GROUPS
    top_count = expert_pick.shape[1]
    capacity = top_count * tok_rows // experts
    flat_ids = (group_pick[:, None] * per_group + expert_pick).reshape(-1)
    onehot = (flat_ids[:, None] == jnp.arange(experts, dtype=jnp.int32)[None, :]).astype(jnp.int32)
    slot_index = jnp.sum(onehot * (jnp.cumsum(onehot, axis=0) - 1), axis=1)
    target = flat_ids * capacity + slot_index
    source = (
        jnp.zeros((experts * capacity,), jnp.int32)
        .at[target]
        .set(jnp.arange(top_count * tok_rows, dtype=jnp.int32) // top_count)
    )
    outgoing = normed[source].reshape(experts, capacity, model_width)
    share = capacity // lax.axis_size("tp")
    start = lax.axis_index("tp") * share
    my_share = lax.dynamic_slice_in_dim(outgoing, start, share, 1)
    landed = lax.all_to_all(my_share, "fs", split_axis=0, concat_axis=1, tiled=True).reshape(
        experts, share, model_width
    )
    arrived = lax.all_gather(landed, "tp", axis=1, tiled=True).reshape(-1, model_width)
    gate_acts = jnp.dot(arrived, gate_new[0], preferred_element_type=jnp.float32)
    up_acts = jnp.dot(arrived, up_new[0], preferred_element_type=jnp.float32)
    hidden = (jax.nn.silu(gate_acts) * up_acts).astype(jnp.bfloat16)
    partial_value = lax.dot_general(
        hidden, down_new[0], (((1,), (1,)), ((), ())), preferred_element_type=jnp.float32
    ).astype(jnp.bfloat16)
    summed = (
        lax.psum_scatter(partial_value, "tp", scatter_dimension=1, tiled=True)
        .astype(jnp.float32)
        .astype(jnp.bfloat16)
    )
    returned = lax.all_to_all(summed, "fs", split_axis=0, concat_axis=0, tiled=True)
    picked = returned[target].reshape(tok_rows, top_count, -1).astype(jnp.float32)
    combined = jnp.sum(route_weight[:, :, None] * picked, axis=1).astype(jnp.bfloat16)
    return (combined, gate_new, up_new, down_new)


def greet(peers):
    barrier = pltpu.get_barrier_semaphore()
    for peer in peers:
        pl.semaphore_signal(barrier, inc=1, device_id=peer, device_id_type=pl.DeviceIdType.MESH)
    pl.semaphore_wait(barrier, len(peers))


def remote(src, dst, send, recv, peer):
    return pltpu.make_async_remote_copy(
        src_ref=src,
        dst_ref=dst,
        send_sem=send,
        recv_sem=recv,
        device_id=peer,
        device_id_type=pl.DeviceIdType.MESH,
    )


def nearest_first(n):
    return [sorted(range(n), key=lambda z, g=g: (abs(z - g), z)) for g in range(n)]


def dot_nt(a, b):
    return lax.dot_general(a, b, (((1,), (1,)), ((), ())), preferred_element_type=jnp.float32)


def fused(tokens, gain, gate, up, down, group_pick, expert_pick, route_weight):
    experts, rows, cols = gate.shape
    tok_rows, width = tokens.shape
    n_fs = lax.axis_size("fs")
    n_gr = lax.axis_size("gr")
    n = GROUPS
    members = experts // n
    cap = tok_rows // n
    half = cap // 2
    out_w = width // 2
    n_w = 3
    table = nearest_first(n)
    bf16, f32, i32 = jnp.bfloat16, jnp.float32, jnp.int32
    lanes = 128

    def kernel(
        tok_in, gain_ref, w_gate, w_up, w_down, gp_ref, ep_ref, rw_ref,
        out, W_own,
        W_other, wf, ow, tok, outgoing, arrived, aw, pin, ownp, home, h, pcol, wout, wcol,
        sends, local, rwz, rwx, rwy, rdx, rdy, rtz, raz, rtt, rat, rp, rh,
    ):
        fs, gr, tp = lax.axis_index("fs"), lax.axis_index("gr"), lax.axis_index("tp")
        g, y = fs // members, fs % members
        other_y, other_x, other_t = 1 - y, 1 - gr, 1 - tp
        hit = [1 - ((g - c + n) % n + n - 1) // n for c in range(n)]
        zs = [sum(table[c][s] * hit[c] for c in range(n)) for s in range(n)]
        x_peer, y_peer, t_peer = {"gr": other_x}, {"fs": g * members + other_y}, {"tp": other_t}
        z_peers = [{"fs": zs[s] * members + y} for s in range(n)]
        started = []

        def send(src, dst, recv, peer):
            copy = remote(src, dst, sends.at[len(started)], recv, peer)
            copy.start()
            started.append(copy)

        def landed(ref, recv):
            remote(ref, ref, sends.at[0], recv, t_peer).wait_recv()

        W = (W_own, W_other)

        def block(j, x, yy, z):
            at = pl.multiple_of((x * n_fs + z * members + yy) * rows, rows)
            return W[j].at[:, pl.ds(at, rows), :]

        w_in = (w_gate, w_up, w_down)
        loads = [
            [
                pltpu.make_async_copy(
                    w_in[w].at[pl.ds(zs[s] * members, members)], wf.at[w, s], local.at[s, w]
                )
                for w in range(n_w)
            ]
            for s in range(n)
        ]
        order = [1, 0] + list(range(2, n))
        for s in order:
            for copy in loads[s]:
                copy.start()
        tok_load = pltpu.make_async_copy(tok_in, tok, local.at[n, 0])
        tok_load.start()
        greet(z_peers[1:] + [x_peer, y_peer, t_peer])

        eye_r = lax.broadcasted_iota(i32, (rows, rows), 0)
        eye_c = lax.broadcasted_iota(i32, (rows, rows), 1)
        gain_col = jnp.sum(jnp.where(eye_r == eye_c, gain_ref[...], 0.0), axis=1, keepdims=True)

        def cast(s, j, w):
            value = wf[w, s, (y + j) % members]
            return ((gain_col * value) if w < 2 else value).astype(bf16)

        for s in order:
            for copy in loads[s]:
                copy.wait()
            for j in range(members):
                for w in range(n_w):
                    if s:
                        ow[s - 1, j, w] = cast(s, j, w)
                    else:
                        at = pl.multiple_of((gr * n_fs + fs) * rows, rows)
                        W[j][w, pl.ds(at, rows), :] = cast(s, j, w)
                if s:
                    send(ow.at[s - 1, j], block(j, gr, y, g), rwz.at[g, j], z_peers[s])
                else:
                    mine = block(j, gr, y, g)
                    send(mine, mine, rwx.at[g, j], x_peer)
                    send(mine, block(1 - j, gr, y, g), rwy.at[g, 1 - j], y_peer)

        gp = gp_ref[...]
        onehot = jnp.where(
            lax.broadcasted_iota(i32, (16, tok_rows), 0) == gp, 1.0, 0.0
        )
        step = 256
        ranks = []
        for c in range(0, tok_rows, step):
            r_i = lax.broadcasted_iota(i32, (tok_rows, step), 0)
            c_i = lax.broadcasted_iota(i32, (tok_rows, step), 1) + c
            before = jnp.dot(
                onehot.astype(bf16),
                jnp.where(r_i < c_i, 1.0, 0.0).astype(bf16),
                preferred_element_type=f32,
            )
            ranks.append(jnp.sum(onehot[:, c : c + step] * before, axis=0, keepdims=True))
        place = gp.astype(f32) * cap + jnp.concatenate(ranks, axis=1)
        l_r = lax.broadcasted_iota(i32, (lanes, lanes), 0)
        l_c = lax.broadcasted_iota(i32, (lanes, lanes), 1)
        eye = l_r == l_c

        def column(row):
            return jnp.sum(jnp.where(eye, row, 0.0), axis=1, keepdims=True)

        for b in range(0, tok_rows, lanes):
            pcol[b : b + lanes, :] = column(place[:, b : b + lanes]).astype(i32)

        for m in range(members):
            value = jnp.zeros((1, tok_rows), f32)
            for k in range(members):
                value += jnp.where(ep_ref[k : k + 1, :] == m, rw_ref[k : k + 1, :], 0.0)
            for b in range(0, tok_rows, lanes):
                wcol[m, b : b + lanes, :] = column(value[:, b : b + lanes])
        place_i = place.astype(i32)

        tok_load.wait()

        def norm(i, _):
            at = pl.ds(pl.multiple_of(i * 64, 64), 64)
            x = tok[at, :].astype(f32)
            scale = lax.rsqrt(jnp.mean(x * x, axis=-1, keepdims=True) + EPS)
            tok[at, :] = (x * scale).astype(bf16)
            return 0

        lax.fori_loop(0, tok_rows // 64, norm, 0)

        first = pl.multiple_of(tp * half, half)
        held = []
        for s in range(n):
            slots = lax.broadcasted_iota(i32, (half, tok_rows), 0) + (zs[s] * cap + tp * half)
            select = jnp.where(slots == place_i, 1.0, 0.0).astype(bf16)
            here = pcol[...] == lax.broadcasted_iota(i32, (tok_rows, half), 1) + (
                zs[s] * cap + tp * half
            )
            weights = jnp.zeros((8, half), f32)
            for m in range(members):
                row = jnp.sum(jnp.where(here, wcol[m], 0.0), axis=0, keepdims=True)
                weights = jnp.where(lax.broadcasted_iota(i32, (8, half), 0) == m, row, weights)
            span = 512
            target = arrived.at[g, pl.ds(first, half)] if s == 0 else outgoing.at[s - 1]

            def pick(c, _, target=target, select=select):
                at = pl.ds(pl.multiple_of(c * span, span), span)
                target[:, at] = jnp.dot(select, tok[:, at], preferred_element_type=f32).astype(bf16)
                return 0

            lax.fori_loop(0, width // span, pick, 0)
            if s == 0:
                aw[g, tp] = weights
                send(target, target, rtt.at[g], t_peer)
                send(aw.at[g, tp], aw.at[g, tp], rat.at[g], t_peer)
            else:
                wout[s - 1] = weights
                held.append((wout.at[s - 1], aw.at[g, tp], raz.at[g], z_peers[s]))
                held.append((target, arrived.at[g, pl.ds(first, half)], rtz.at[g], z_peers[s]))

        def relay(s):
            from_x, from_y = block(1, other_x, y, zs[s]), block(1, gr, other_y, zs[s])
            landed(from_x, rwx.at[zs[s], 1])
            send(from_x, block(0, other_x, y, zs[s]), rdy.at[zs[s]], y_peer)
            landed(from_y, rwy.at[zs[s], 1])
            send(from_y, from_y, rdx.at[zs[s]], x_peer)

        for s in range(1, n):
            for j in range(members):
                mine = block(j, gr, y, zs[s])
                landed(mine, rwz.at[zs[s], j])
                send(mine, mine, rwx.at[zs[s], j], x_peer)
                send(mine, block(1 - j, gr, y, zs[s]), rwy.at[zs[s], 1 - j], y_peer)
            if s == n - 1:
                for copy in held:
                    send(*copy)
            relay(s - 1)
        relay(n - 1)

        def forward(s):
            slot, small = arrived.at[zs[s], pl.ds(first, half)], aw.at[zs[s], tp]
            landed(slot, rtz.at[zs[s]])
            send(slot, slot, rtt.at[zs[s]], t_peer)
            landed(small, raz.at[zs[s]])
            send(small, small, rat.at[zs[s]], t_peer)

        forward(1)
        for s in range(n):
            landed(block(0, other_x, y, zs[s]), rwx.at[zs[s], 0])
            landed(block(0, gr, other_y, zs[s]), rwy.at[zs[s], 0])
            landed(block(1, other_x, other_y, zs[s]), rdx.at[zs[s]])
            landed(block(0, other_x, other_y, zs[s]), rdy.at[zs[s]])
        piece = 512
        second = pl.multiple_of(other_t * half, half)

        def chunk(s):
            z = zs[s]
            if s > 1:
                forward(s)
            landed(arrived.at[z, pl.ds(second, half)], rtt.at[z])
            landed(aw.at[z, other_t], rat.at[z])

            for j in range(members):
                member = (y + j) % members
                rows_in = arrived[z]
                gate_acts = jnp.dot(rows_in, W[j][0], preferred_element_type=f32)
                up_acts = jnp.dot(rows_in, W[j][1], preferred_element_type=f32)
                value = gate_acts / (1.0 + jnp.exp(-gate_acts)) * up_acts
                for t in range(2):
                    scale = column(aw[z, t, pl.ds(member, 1), :])
                    at = slice(t * half, (t + 1) * half)
                    h[j, at, :] = (value[at] * scale).astype(bf16)

            def down_rows(base, c):
                at = pl.ds(pl.multiple_of(base + c * piece, piece), piece)
                return dot_nt(h[0], W_own[2, at, :]) + dot_nt(h[1], W_other[2, at, :])

            give = tok.at[pl.ds(s * cap, cap), pl.ds(0, out_w)]
            back = tok.at[pl.ds(s * cap, cap), pl.ds(out_w, out_w)]

            def theirs(c, _):
                at = pl.ds(pl.multiple_of(c * piece, piece), piece)
                give[:, at] = down_rows(other_t * out_w, c).astype(bf16)
                return 0

            def ours(c, _):
                at = pl.ds(pl.multiple_of(c * piece, piece), piece)
                ownp[:, at] = down_rows(tp * out_w, c).astype(bf16).astype(f32)
                return 0

            lax.fori_loop(0, out_w // piece, theirs, 0)
            send(give, pin.at[s], rp.at[s], t_peer)
            lax.fori_loop(0, out_w // piece, ours, 0)
            landed(pin.at[s], rp.at[s])
            total = (ownp[...] + pin[s].astype(f32)).astype(bf16)
            if s:
                back[...] = total
                send(back, home.at[g], rh.at[g], z_peers[s])
            else:
                home[g] = total

        def restore(s):
            z = zs[s]

            def rows_of(b, _):
                at = pl.ds(pl.multiple_of(b * 256, 256), 256)
                slots = lax.broadcasted_iota(i32, (256, cap), 1) + z * cap
                back = jnp.where(slots == pcol[at, :], 1.0, 0.0).astype(bf16)
                value = jnp.dot(back, home[z], preferred_element_type=f32)
                if s:
                    value += out[at, :].astype(f32)
                out[at, :] = value.astype(bf16)
                return 0

            lax.fori_loop(0, tok_rows // 256, rows_of, 0)

        for s in [1, 2, 0] + list(range(3, n)):
            chunk(s)
        for s in range(n):
            if s:
                landed(home.at[zs[s]], rh.at[zs[s]])
            restore(s)
        for copy in started:
            copy.wait_send()

    n_sends = (
        (n - 1) * members + 2 * members
        + 2 * n
        + (n - 1) * 2 * members + 2 * n
        + 2 * (n - 1)
        + n + n - 1
    )
    dma = pltpu.SemaphoreType.DMA
    vmem = pltpu.VMEM
    any_space = pl.BlockSpec(memory_space=pl.ANY)
    in_vmem = pl.BlockSpec(memory_space=pltpu.VMEM)
    return pl.pallas_call(
        kernel,
        out_shape=(vmem((tok_rows, out_w), bf16), vmem((n_w, width, cols), bf16)),
        in_specs=[any_space, in_vmem, any_space, any_space, any_space] + [in_vmem] * 3,
        out_specs=(in_vmem, in_vmem),
        scratch_shapes=[
            vmem((n_w, width, cols), bf16),
            vmem((n_w, n, members, rows, cols), f32),
            vmem((n - 1, members, n_w, rows, cols), bf16),
            vmem((tok_rows, width), bf16),
            vmem((n - 1, half, width), bf16),
            vmem((n, cap, width), bf16),
            vmem((n, 2, 8, lanes), f32),
            vmem((n, cap, out_w), bf16),
            vmem((cap, out_w), f32),
            vmem((n, cap, out_w), bf16),
            vmem((members, cap, cols), bf16),
            vmem((tok_rows, 1), i32),
            vmem((n - 1, 8, lanes), f32),
            vmem((members, tok_rows, 1), f32),
            dma((n_sends,)),
            dma((n + 1, n_w)),
            dma((n, members)),
            dma((n, members)),
            dma((n, members)),
            dma((n,)),
            dma((n,)),
            dma((n,)),
            dma((n,)),
            dma((n,)),
            dma((n,)),
            dma((n,)),
            dma((n,)),
        ],
        compiler_params=pltpu.CompilerParams(
            collective_id=0, has_side_effects=True, vmem_limit_bytes=51 * 2**20
        ),
        name="fused",
    )(
        tokens, gain[None, :], gate, up, down,
        group_pick[None, :], expert_pick.T, route_weight.T,
    )


def deliver(combined, served):
    parts = 4
    n_w, width, cols = served.shape

    def kernel(src, weights, out, gate, up, down, sems):
        copies = []
        for w, dst in enumerate((gate, up, down)):
            step = width // parts
            for p in range(parts):
                at = pl.ds(p * step, step)
                copies.append(
                    pltpu.make_async_copy(weights.at[w, at], dst.at[at], sems.at[len(copies)])
                )
        step = src.shape[0] // parts
        for p in range(parts):
            at = pl.ds(p * step, step)
            copies.append(pltpu.make_async_copy(src.at[at], out.at[at], sems.at[len(copies)]))
        for copy in copies:
            copy.start()
        for copy in copies:
            copy.wait()

    serve = jax.ShapeDtypeStruct((width, cols), served.dtype)
    return pl.pallas_call(
        kernel,
        out_shape=(jax.ShapeDtypeStruct(combined.shape, combined.dtype), serve, serve, serve),
        in_specs=[pl.BlockSpec(memory_space=pltpu.VMEM)] * 2,
        out_specs=[pl.BlockSpec(memory_space=pl.ANY)] * 4,
        scratch_shapes=[pltpu.SemaphoreType.DMA(((n_w + 1) * parts,))],
        compiler_params=pltpu.CompilerParams(vmem_limit_bytes=12 * 2**20),
        name="deliver",
    )(combined, served)


def local_whole_group(*args):
    combined, gate_new, up_new, down_new = deliver(*fused(*args))
    return (combined, gate_new[None], up_new[None], down_new[None])


def local(tokens, norm_gain, gate, up, down, group_pick, expert_pick, route_weight):
    per_group = gate.shape[0] // GROUPS
    fits = (
        per_group == expert_pick.shape[1] == 2
        and lax.axis_size("gr") == lax.axis_size("tp") == 2
        and lax.axis_size("fs") == gate.shape[0]
        and tokens.shape[0] == 2 * GROUPS * 128
    )
    body = local_whole_group if fits else local_spread
    return body(tokens, norm_gain, gate, up, down, group_pick, expert_pick, route_weight)


def solution(mesh):
    in_specs = (
        P(("gr", "fs"), None),
        P(("gr", "fs")),
        P(None, ("gr", "fs"), "tp"),
        P(None, ("gr", "fs"), "tp"),
        P(None, ("gr", "fs"), "tp"),
        P(("gr", "fs")),
        P(("gr", "fs"), None),
        P(("gr", "fs"), None),
    )
    out_specs = (
        P(("gr", "fs"), "tp"),
        P("fs", None, "tp"),
        P("fs", None, "tp"),
        P("fs", None, "tp"),
    )
    return jax.shard_map(local, mesh=mesh, in_specs=in_specs, out_specs=out_specs, check_vma=False)
```

```python
import jax
import jax.numpy as jnp
from jax import lax
from jax.experimental import pallas as pl
from jax.experimental.pallas import tpu as pltpu
from jax.sharding import PartitionSpec as P

GROUPS = 4


EPS = 1e-06


def local_spread(
    tokens, norm_gain, gate_weight, up_weight, down_weight, group_pick, expert_pick, route_weight
):
    scaled = norm_gain[None, :, None]
    gate_local = (scaled * gate_weight).astype(jnp.bfloat16)
    up_local = (scaled * up_weight).astype(jnp.bfloat16)
    down_local = down_weight.astype(jnp.bfloat16)
    experts, rows_dev, cols_dev = gate_local.shape
    gate_four = gate_local.reshape(experts, 1, rows_dev, cols_dev)
    up_four = up_local.reshape(experts, 1, rows_dev, cols_dev)
    down_four = down_local.reshape(experts, 1, rows_dev, cols_dev)
    gathered = (
        lax.all_gather(gate_four, "gr", axis=1, tiled=True),
        lax.all_gather(up_four, "gr", axis=1, tiled=True),
        lax.all_gather(down_four, "gr", axis=1, tiled=True),
    )
    relaid = (
        lax.all_to_all(gathered[0], "fs", split_axis=0, concat_axis=2, tiled=True),
        lax.all_to_all(gathered[1], "fs", split_axis=0, concat_axis=2, tiled=True),
        lax.all_to_all(gathered[2], "fs", split_axis=0, concat_axis=2, tiled=True),
    )
    gate_new = relaid[0].reshape(1, -1, cols_dev)
    up_new = relaid[1].reshape(1, -1, cols_dev)
    down_new = relaid[2].reshape(1, -1, cols_dev)
    tok_rows, model_width = tokens.shape
    as_float = tokens.astype(jnp.float32)
    normed = (
        as_float * lax.rsqrt(jnp.mean(as_float * as_float, axis=-1, keepdims=True) + EPS)
    ).astype(jnp.bfloat16)
    per_group = experts // GROUPS
    top_count = expert_pick.shape[1]
    capacity = top_count * tok_rows // experts
    flat_ids = (group_pick[:, None] * per_group + expert_pick).reshape(-1)
    onehot = (flat_ids[:, None] == jnp.arange(experts, dtype=jnp.int32)[None, :]).astype(jnp.int32)
    slot_index = jnp.sum(onehot * (jnp.cumsum(onehot, axis=0) - 1), axis=1)
    target = flat_ids * capacity + slot_index
    source = (
        jnp.zeros((experts * capacity,), jnp.int32)
        .at[target]
        .set(jnp.arange(top_count * tok_rows, dtype=jnp.int32) // top_count)
    )
    outgoing = normed[source].reshape(experts, capacity, model_width)
    share = capacity // lax.axis_size("tp")
    start = lax.axis_index("tp") * share
    my_share = lax.dynamic_slice_in_dim(outgoing, start, share, 1)
    landed = lax.all_to_all(my_share, "fs", split_axis=0, concat_axis=1, tiled=True).reshape(
        experts, share, model_width
    )
    arrived = lax.all_gather(landed, "tp", axis=1, tiled=True).reshape(-1, model_width)
    gate_acts = jnp.dot(arrived, gate_new[0], preferred_element_type=jnp.float32)
    up_acts = jnp.dot(arrived, up_new[0], preferred_element_type=jnp.float32)
    hidden = (jax.nn.silu(gate_acts) * up_acts).astype(jnp.bfloat16)
    partial_value = lax.dot_general(
        hidden, down_new[0], (((1,), (1,)), ((), ())), preferred_element_type=jnp.float32
    ).astype(jnp.bfloat16)
    summed = (
        lax.psum_scatter(partial_value, "tp", scatter_dimension=1, tiled=True)
        .astype(jnp.float32)
        .astype(jnp.bfloat16)
    )
    returned = lax.all_to_all(summed, "fs", split_axis=0, concat_axis=0, tiled=True)
    picked = returned[target].reshape(tok_rows, top_count, -1).astype(jnp.float32)
    combined = jnp.sum(route_weight[:, :, None] * picked, axis=1).astype(jnp.bfloat16)
    return (combined, gate_new, up_new, down_new)


def greet(peers):
    barrier = pltpu.get_barrier_semaphore()
    for peer in peers:
        pl.semaphore_signal(barrier, inc=1, device_id=peer, device_id_type=pl.DeviceIdType.MESH)
    return lambda: pl.semaphore_wait(barrier, len(peers))


def remote(src, dst, send, recv, peer):
    return pltpu.make_async_remote_copy(
        src_ref=src,
        dst_ref=dst,
        send_sem=send,
        recv_sem=recv,
        device_id=peer,
        device_id_type=pl.DeviceIdType.MESH,
    )


def nearest_first(n):
    return [sorted(range(n), key=lambda z, g=g: (abs(z - g), z)) for g in range(n)]


def dot_nt(a, b):
    return lax.dot_general(a, b, (((1,), (1,)), ((), ())), preferred_element_type=jnp.float32)


def fused(tokens, gain, gate, up, down, group_pick, expert_pick, route_weight):
    experts, rows, cols = gate.shape
    tok_rows, width = tokens.shape
    n_fs = lax.axis_size("fs")
    n_gr = lax.axis_size("gr")
    n = GROUPS
    members = experts // n
    cap = tok_rows // n
    half = cap // 2
    out_w = width // 2
    n_w = 3
    table = nearest_first(n)
    bf16, f32, i32 = jnp.bfloat16, jnp.float32, jnp.int32
    lanes = 128
    piece = 512

    def kernel(
        tok_in, gain_ref, w_gate, w_up, w_down, gp_ref, ep_ref, rw_ref,
        out, W_own,
        W_other, wf, ow, tok, outgoing, arrived, aw, pin, ownp, home, h, pcol, wout, wcol, mask,
        sends, local, rwz, rwx, rwy, rdx, rdy, rtz, raz, rtt, rat, rp, rh,
    ):
        fs, gr, tp = lax.axis_index("fs"), lax.axis_index("gr"), lax.axis_index("tp")
        g, y = fs // members, fs % members
        other_y, other_x, other_t = 1 - y, 1 - gr, 1 - tp
        hit = [1 - ((g - c + n) % n + n - 1) // n for c in range(n)]
        zs = [sum(table[c][s] * hit[c] for c in range(n)) for s in range(n)]
        x_peer, y_peer, t_peer = {"gr": other_x}, {"fs": g * members + other_y}, {"tp": other_t}
        z_peers = [{"fs": zs[s] * members + y} for s in range(n)]
        started = []

        def send(src, dst, recv, peer):
            copy = remote(src, dst, sends.at[len(started)], recv, peer)
            copy.start()
            started.append(copy)

        def landed(ref, recv):
            remote(ref, ref, sends.at[0], recv, t_peer).wait_recv()

        W = (W_own, W_other)

        def block(j, x, yy, z):
            at = pl.multiple_of((x * n_fs + z * members + yy) * rows, rows)
            return W[j].at[:, pl.ds(at, rows), :]

        all_here = greet(z_peers[1:] + [x_peer, y_peer, t_peer])
        w_in = (w_gate, w_up, w_down)
        loads = [
            [
                pltpu.make_async_copy(
                    w_in[w].at[pl.ds(zs[s] * members, members)], wf.at[w, s], local.at[s, w]
                )
                for w in range(n_w)
            ]
            for s in range(n)
        ]
        order = [1, 0] + list(range(2, n))
        for s in order:
            for copy in loads[s]:
                copy.start()
        tok_load = pltpu.make_async_copy(tok_in, tok, local.at[n, 0])
        tok_load.start()
        eye_r = lax.broadcasted_iota(i32, (rows, rows), 0)
        eye_c = lax.broadcasted_iota(i32, (rows, rows), 1)
        gain_col = jnp.sum(jnp.where(eye_r == eye_c, gain_ref[...], 0.0), axis=1, keepdims=True)

        def cast(s, j, w):
            value = wf[w, s, (y + j) % members]
            return ((gain_col * value) if w < 2 else value).astype(bf16)

        def make(s):
            for copy in loads[s]:
                copy.wait()
            for j in range(members):
                for w in range(n_w):
                    if s:
                        ow[s - 1, j, w] = cast(s, j, w)
                    else:
                        at = pl.multiple_of((gr * n_fs + fs) * rows, rows)
                        W[j][w, pl.ds(at, rows), :] = cast(s, j, w)

        for s in order:
            make(s)
        all_here()
        for s in order:
            for j in range(members):
                if s:
                    send(ow.at[s - 1, j], block(j, gr, y, g), rwz.at[g, j], z_peers[s])
                else:
                    mine = block(j, gr, y, g)
                    send(mine, mine, rwx.at[g, j], x_peer)
                    send(mine, block(1 - j, gr, y, g), rwy.at[g, 1 - j], y_peer)

        gp = gp_ref[...]
        onehot = jnp.where(
            lax.broadcasted_iota(i32, (16, tok_rows), 0) == gp, 1.0, 0.0
        )
        step = 256
        ranks = []
        for c in range(0, tok_rows, step):
            r_i = lax.broadcasted_iota(i32, (tok_rows, step), 0)
            c_i = lax.broadcasted_iota(i32, (tok_rows, step), 1) + c
            before = jnp.dot(
                onehot.astype(bf16),
                jnp.where(r_i < c_i, 1.0, 0.0).astype(bf16),
                preferred_element_type=f32,
            )
            ranks.append(jnp.sum(onehot[:, c : c + step] * before, axis=0, keepdims=True))
        place = gp.astype(f32) * cap + jnp.concatenate(ranks, axis=1)
        l_r = lax.broadcasted_iota(i32, (lanes, lanes), 0)
        l_c = lax.broadcasted_iota(i32, (lanes, lanes), 1)
        eye = l_r == l_c

        def column(row):
            return jnp.sum(jnp.where(eye, row, 0.0), axis=1, keepdims=True)

        for b in range(0, tok_rows, lanes):
            pcol[b : b + lanes, :] = column(place[:, b : b + lanes]).astype(i32)

        for m in range(members):
            value = jnp.zeros((1, tok_rows), f32)
            for k in range(members):
                value += jnp.where(ep_ref[k : k + 1, :] == m, rw_ref[k : k + 1, :], 0.0)
            for b in range(0, tok_rows, lanes):
                wcol[m, b : b + lanes, :] = column(value[:, b : b + lanes])
        place_i = place.astype(i32)

        tok_load.wait()

        def norm(i, _):
            at = pl.ds(pl.multiple_of(i * 64, 64), 64)
            x = tok[at, :].astype(f32)
            scale = lax.rsqrt(jnp.mean(x * x, axis=-1, keepdims=True) + EPS)
            tok[at, :] = (x * scale).astype(bf16)
            return 0

        lax.fori_loop(0, tok_rows // 64, norm, 0)

        first = pl.multiple_of(tp * half, half)
        held = []
        for s in range(n):
            slots = lax.broadcasted_iota(i32, (half, tok_rows), 0) + (zs[s] * cap + tp * half)
            select = jnp.where(slots == place_i, 1.0, 0.0).astype(bf16)
            here = pcol[...] == lax.broadcasted_iota(i32, (tok_rows, half), 1) + (
                zs[s] * cap + tp * half
            )
            weights = jnp.zeros((8, half), f32)
            for m in range(members):
                row = jnp.sum(jnp.where(here, wcol[m], 0.0), axis=0, keepdims=True)
                weights = jnp.where(lax.broadcasted_iota(i32, (8, half), 0) == m, row, weights)
            span = 512
            target = arrived.at[g, pl.ds(first, half)] if s == 0 else outgoing.at[s - 1]

            def pick(c, _, target=target, select=select):
                at = pl.ds(pl.multiple_of(c * span, span), span)
                target[:, at] = jnp.dot(select, tok[:, at], preferred_element_type=f32).astype(bf16)
                return 0

            lax.fori_loop(0, width // span, pick, 0)
            if s == 0:
                aw[g, tp] = weights
                send(target, target, rtt.at[g], t_peer)
                send(aw.at[g, tp], aw.at[g, tp], rat.at[g], t_peer)
            else:
                wout[s - 1] = weights
                held.append((wout.at[s - 1], aw.at[g, tp], raz.at[g], z_peers[s]))
                held.append((target, arrived.at[g, pl.ds(first, half)], rtz.at[g], z_peers[s]))

        def relay(s):
            from_x, from_y = block(1, other_x, y, zs[s]), block(1, gr, other_y, zs[s])
            landed(from_x, rwx.at[zs[s], 1])
            send(from_x, block(0, other_x, y, zs[s]), rdy.at[zs[s]], y_peer)
            landed(from_y, rwy.at[zs[s], 1])
            send(from_y, from_y, rdx.at[zs[s]], x_peer)

        for s in range(1, n):
            for j in range(members):
                mine = block(j, gr, y, zs[s])
                landed(mine, rwz.at[zs[s], j])
                send(mine, mine, rwx.at[zs[s], j], x_peer)
                send(mine, block(1 - j, gr, y, zs[s]), rwy.at[zs[s], 1 - j], y_peer)
            if s == n - 1:
                for copy in held:
                    send(*copy)
            relay(s - 1)
        relay(n - 1)

        def forward(s):
            slot, small = arrived.at[zs[s], pl.ds(first, half)], aw.at[zs[s], tp]
            landed(slot, rtz.at[zs[s]])
            send(slot, slot, rtt.at[zs[s]], t_peer)
            landed(small, raz.at[zs[s]])
            send(small, small, rat.at[zs[s]], t_peer)

        forward(1)
        for s in range(n):
            landed(block(0, other_x, y, zs[s]), rwx.at[zs[s], 0])
            landed(block(0, gr, other_y, zs[s]), rwy.at[zs[s], 0])
            landed(block(1, other_x, other_y, zs[s]), rdx.at[zs[s]])
            landed(block(0, other_x, other_y, zs[s]), rdy.at[zs[s]])
        second = pl.multiple_of(other_t * half, half)

        def chunk(s):
            z = zs[s]
            if s > 1:
                forward(s)
            landed(arrived.at[z, pl.ds(second, half)], rtt.at[z])
            landed(aw.at[z, other_t], rat.at[z])

            for j in range(members):
                member = (y + j) % members
                rows_in = arrived[z]
                gate_acts = jnp.dot(rows_in, W[j][0], preferred_element_type=f32)
                up_acts = jnp.dot(rows_in, W[j][1], preferred_element_type=f32)
                value = gate_acts / (1.0 + jnp.exp(-gate_acts)) * up_acts
                for t in range(2):
                    scale = column(aw[z, t, pl.ds(member, 1), :])
                    at = slice(t * half, (t + 1) * half)
                    h[j, at, :] = (value[at] * scale).astype(bf16)

            def down_rows(base, c):
                at = pl.ds(pl.multiple_of(base + c * piece, piece), piece)
                return dot_nt(h[0], W_own[2, at, :]) + dot_nt(h[1], W_other[2, at, :])

            give = tok.at[pl.ds(s * cap, cap), pl.ds(0, out_w)]
            back = tok.at[pl.ds(s * cap, cap), pl.ds(out_w, out_w)]

            def theirs(c, _):
                at = pl.ds(pl.multiple_of(c * piece, piece), piece)
                give[:, at] = down_rows(other_t * out_w, c).astype(bf16)
                return 0

            def ours(c, _):
                at = pl.ds(pl.multiple_of(c * piece, piece), piece)
                ownp[:, at] = down_rows(tp * out_w, c).astype(bf16).astype(f32)
                return 0

            lax.fori_loop(0, out_w // piece, theirs, 0)
            send(give, pin.at[s], rp.at[s], t_peer)
            lax.fori_loop(0, out_w // piece, ours, 0)
            landed(pin.at[s], rp.at[s])
            total = (ownp[...] + pin[s].astype(f32)).astype(bf16)
            if s:
                back[...] = total
                for c in range(out_w // piece):
                    at = pl.ds(c * piece, piece)
                    send(back.at[:, at], home.at[g, :, at], rh.at[g, c], z_peers[s])
            else:
                home[g] = total

        def slots_of(z, at):
            slots = lax.broadcasted_iota(i32, (256, cap), 1) + z * cap
            return jnp.where(slots == pcol[at, :], 1.0, 0.0).astype(bf16)

        def find(s):
            def rows_of(b, _):
                at = pl.ds(pl.multiple_of(b * 256, 256), 256)
                mask[at, :] = slots_of(zs[s], at)
                return 0

            lax.fori_loop(0, tok_rows // 256, rows_of, 0)

        def restore(s, c):
            z = zs[s]
            cols_at = pl.ds(c * piece, piece)

            def rows_of(b, _):
                at = pl.ds(pl.multiple_of(b * 256, 256), 256)
                value = jnp.dot(mask[at, :], home[z, :, cols_at], preferred_element_type=f32)
                if s:
                    value += out[at, cols_at].astype(f32)
                out[at, cols_at] = value.astype(bf16)
                return 0

            lax.fori_loop(0, tok_rows // 256, rows_of, 0)

        for s in [1, 2, 0] + list(range(3, n)):
            chunk(s)
        for s in [0, 1] + list(range(n - 1, 1, -1)):
            find(s)
            for c in range(out_w // piece):
                if s:
                    landed(home.at[zs[s], :, pl.ds(c * piece, piece)], rh.at[zs[s], c])
                restore(s, c)
        for copy in started:
            copy.wait_send()

    n_sends = (
        (n - 1) * members + 2 * members
        + 2 * n
        + (n - 1) * 2 * members + 2 * n
        + 2 * (n - 1)
        + n + (n - 1) * (out_w // piece)
    )
    dma = pltpu.SemaphoreType.DMA
    vmem = pltpu.VMEM
    any_space = pl.BlockSpec(memory_space=pl.ANY)
    in_vmem = pl.BlockSpec(memory_space=pltpu.VMEM)
    return pl.pallas_call(
        kernel,
        out_shape=(vmem((tok_rows, out_w), bf16), vmem((n_w, width, cols), bf16)),
        in_specs=[any_space, in_vmem, any_space, any_space, any_space] + [in_vmem] * 3,
        out_specs=(in_vmem, in_vmem),
        scratch_shapes=[
            vmem((n_w, width, cols), bf16),
            vmem((n_w, n, members, rows, cols), f32),
            vmem((n - 1, members, n_w, rows, cols), bf16),
            vmem((tok_rows, width), bf16),
            vmem((n - 1, half, width), bf16),
            vmem((n, cap, width), bf16),
            vmem((n, 2, 8, lanes), f32),
            vmem((n, cap, out_w), bf16),
            vmem((cap, out_w), f32),
            vmem((n, cap, out_w), bf16),
            vmem((members, cap, cols), bf16),
            vmem((tok_rows, 1), i32),
            vmem((n - 1, 8, lanes), f32),
            vmem((members, tok_rows, 1), f32),
            vmem((tok_rows, cap), bf16),
            dma((n_sends,)),
            dma((n + 1, n_w)),
            dma((n, members)),
            dma((n, members)),
            dma((n, members)),
            dma((n,)),
            dma((n,)),
            dma((n,)),
            dma((n,)),
            dma((n,)),
            dma((n,)),
            dma((n,)),
            dma((n, out_w // piece)),
        ],
        compiler_params=pltpu.CompilerParams(
            collective_id=0, has_side_effects=True, vmem_limit_bytes=51 * 2**20
        ),
        name="fused",
    )(
        tokens, gain[None, :], gate, up, down,
        group_pick[None, :], expert_pick.T, route_weight.T,
    )


def deliver(combined, served):
    parts = 4
    n_w, width, cols = served.shape

    def kernel(src, weights, out, gate, up, down, sems):
        copies = []
        for w, dst in enumerate((gate, up, down)):
            step = width // parts
            for p in range(parts):
                at = pl.ds(p * step, step)
                copies.append(
                    pltpu.make_async_copy(weights.at[w, at], dst.at[at], sems.at[len(copies)])
                )
        step = src.shape[0] // parts
        for p in range(parts):
            at = pl.ds(p * step, step)
            copies.append(pltpu.make_async_copy(src.at[at], out.at[at], sems.at[len(copies)]))
        for copy in copies:
            copy.start()
        for copy in copies:
            copy.wait()

    serve = jax.ShapeDtypeStruct((width, cols), served.dtype)
    return pl.pallas_call(
        kernel,
        out_shape=(jax.ShapeDtypeStruct(combined.shape, combined.dtype), serve, serve, serve),
        in_specs=[pl.BlockSpec(memory_space=pltpu.VMEM)] * 2,
        out_specs=[pl.BlockSpec(memory_space=pl.ANY)] * 4,
        scratch_shapes=[pltpu.SemaphoreType.DMA(((n_w + 1) * parts,))],
        compiler_params=pltpu.CompilerParams(vmem_limit_bytes=12 * 2**20),
        name="deliver",
    )(combined, served)


def local_whole_group(*args):
    combined, gate_new, up_new, down_new = deliver(*fused(*args))
    return (combined, gate_new[None], up_new[None], down_new[None])


def local(tokens, norm_gain, gate, up, down, group_pick, expert_pick, route_weight):
    per_group = gate.shape[0] // GROUPS
    fits = (
        per_group == expert_pick.shape[1] == 2
        and lax.axis_size("gr") == lax.axis_size("tp") == 2
        and lax.axis_size("fs") == gate.shape[0]
        and tokens.shape[0] == 2 * GROUPS * 128
    )
    body = local_whole_group if fits else local_spread
    return body(tokens, norm_gain, gate, up, down, group_pick, expert_pick, route_weight)


def solution(mesh):
    in_specs = (
        P(("gr", "fs"), None),
        P(("gr", "fs")),
        P(None, ("gr", "fs"), "tp"),
        P(None, ("gr", "fs"), "tp"),
        P(None, ("gr", "fs"), "tp"),
        P(("gr", "fs")),
        P(("gr", "fs"), None),
        P(("gr", "fs"), None),
    )
    out_specs = (
        P(("gr", "fs"), "tp"),
        P("fs", None, "tp"),
        P("fs", None, "tp"),
        P("fs", None, "tp"),
    )
    return jax.shard_map(local, mesh=mesh, in_specs=in_specs, out_specs=out_specs, check_vma=False)
```
